128 devices in a mesh: sp: 64 (over z, y, x), tp: 2 (over core).
Axes of the slice: x: 4, y: 4, z: 4, core: 2. Of those that a mesh axis runs over, the one named last changes fastest.
Arguments:
- queries: bfloat16 [16384, 1024], P('sp', 'tp'), may hold values from -100 to 100
- keys: bfloat16 [256, 16384], P('tp', 'sp'), may hold values from -5 to 5
- values: bfloat16 [256, 16384], P('tp', 'sp'), may hold values from -4.5 to 4.5
- gate_cache: float32 [8, 16384], P('tp', 'sp'), as said below
- documents: int32 [16384], P('sp'), may hold values from 0 to 2, never falling along the last dimension, each value on 1 to 10240 neighbouring positions
- residual: bfloat16 [16384, 2048], P(('sp', 'tp')), may hold values from -3 to 3
- out_weight: bfloat16 [1024, 2048], replicated, may hold values from -2 to 2
- mix_gain: bfloat16 [2048], replicated, may hold values from 0.099609375 to 1.8984375
- routes: int32 [16384, 4], P(('sp', 'tp')), may hold values from 0 to 127, all different within a row; in each aligned block of 128 rows (0 to 127, 128 to 255, ...) at most 8 rows name the same one
- route_weight: float32 [16384, 4], P(('sp', 'tp')), may hold values from 0.25 to 1
- expert_gate: bfloat16 [128, 2048, 512], P(('sp', 'tp')), may hold values from -0.125 to 0.125
- expert_up: bfloat16 [128, 2048, 512], P(('sp', 'tp')), may hold values from -0.125 to 0.125
- expert_down: bfloat16 [128, 512, 2048], P(('sp', 'tp')), may hold values from -0.25 to 0.25
- shared_gate: bfloat16 [2048, 512], replicated, may hold values from -0.125 to 0.125
- shared_up: bfloat16 [2048, 512], replicated, may hold values from -0.125 to 0.125
- shared_down: bfloat16 [512, 2048], replicated, may hold values from -0.25 to 0.25
- ffn_gain: bfloat16 [2048], replicated, may hold values from 0.099609375 to 1.8984375
Outputs:
- result: bfloat16 [16384, 2048], P(('sp', 'tp'))
The draws below stay inside these ranges and needn't reach their ends.
Inputs may be any that keep to these rules, and one draw needn't show every extreme that they name: `gate_cache`: entry (h, j) is the sum of head h's log forget gates over positions 0 to j. `documents`: never falls along the positions; no document has more than 10240 positions. `routes`: each row names 4 different experts; in the rows of one device (aligned blocks of 128 rows) no expert is named more than 8 times, a bound that some block reaches.
All inputs are finite; a program needn't handle non-finite values.
Results may differ from the reference program's by a relative error of at most 0.013.
Values may be sent and summed in bfloat16 or wider, within the bound.
No kernel may reach another device: no remote copies, remote signals or barrier semaphores. Data moves between devices by JAX's collectives and lax.ppermute only.
A program may use at most 256 MiB of HBM per device.

```python
import math
import jax
import jax.numpy as jnp
import numpy as np
from jax import lax

D = 2048
HEADS = 8
KV_HEADS = 2
HD = 128
EFF = 512
SFF = 512
TOPK = 4
DOCS = 3
TOK_DEV = 256
SEQUENCE_TOKENS = 16384
ROWS = 128
EXPERTS = 128
CAP = 8
DOC_MOST = 10240


def attention_draw(key):
    sequence_pieces = jax.random.split(jax.random.fold_in(key, 7), 2)
    key_rows = jnp.clip(jax.random.normal(sequence_pieces[0], (KV_HEADS, HD, SEQUENCE_TOKENS), jnp.float32), -4.5, 4.5)
    query_rows = jnp.clip(jax.random.normal(sequence_pieces[1], (SEQUENCE_TOKENS, HEADS, HD), jnp.float32), -4.5, 4.5)
    return (query_rows.reshape(SEQUENCE_TOKENS, HEADS * HD), key_rows.reshape(KV_HEADS * HD, SEQUENCE_TOKENS))


def draw_queries(key, part):
    return attention_draw(key)[0].astype(jnp.bfloat16)


def draw_keys(key, part):
    return attention_draw(key)[1].astype(jnp.bfloat16)


def draw_gate_cache(key, part):
    sequence_pieces = jax.random.split(jax.random.fold_in(key, 11), 7)
    ordering = jax.random.permutation(sequence_pieces[0], HEADS)
    fast_count = HEADS // 2
    is_fast = ordering < fast_count
    blocks = SEQUENCE_TOKENS // TOK_DEV
    block_rate = jnp.exp(jax.random.uniform(sequence_pieces[1], (HEADS, blocks), jnp.float32, -0.7, 0.7))
    block_rate = jnp.repeat(block_rate, TOK_DEV, axis=1)
    roughness = jax.random.uniform(sequence_pieces[2], (HEADS, SEQUENCE_TOKENS), jnp.float32, 0.2, 1.8)
    slow_rate = jax.random.uniform(sequence_pieces[3], (HEADS, 1), jnp.float32, 0.3, 0.7) / SEQUENCE_TOKENS
    fast_rate = 1.0 / jax.random.uniform(sequence_pieces[4], (HEADS, 1), jnp.float32, 30.0, 100.0)
    decay_rates = jnp.where(is_fast[:, None], fast_rate, slow_rate) * block_rate * roughness
    surge_position = jax.random.randint(sequence_pieces[5], (3,), 0, SEQUENCE_TOKENS)
    token_surges = jnp.any(jnp.arange(SEQUENCE_TOKENS)[None, :] == surge_position[:, None], axis=0)
    loss_values = -jnp.log(1.0 - jax.random.uniform(sequence_pieces[6], (HEADS, 1), jnp.float32, 0.2, 0.35))
    gate_logarithms = -decay_rates - jnp.where(token_surges[None, :], loss_values, 0.0)
    return jnp.cumsum(gate_logarithms, axis=1)


def steps_of(stream_key, extent, pieces, low, high):
    factor_of, own = 1.0, jax.random.fold_in(stream_key, 6)
    for position, shards_of in pieces:
        steps = jnp.exp(jax.random.uniform(jax.random.fold_in(own, position), (shards_of,), jnp.float32, low / len(pieces), high / len(pieces)))
        factor_of = factor_of * jnp.repeat(steps, extent[position] // shards_of).reshape([-1 if axis == position else 1 for axis in range(len(extent))])
    return factor_of


def length_profile(count, total, bound, slope):
    loads = [(1 << 20) // math.isqrt(grade ** slope) + 1 for grade in range(2, count + 1)]
    spare, holding = total - bound - (count - 1), [1] * (count - 1)
    while spare > 0:
        movable = [i for i in range(count - 1) if holding[i] < bound]
        whole, left = sum([loads[i] for i in movable]), spare
        for i in movable:
            addition = min(bound - holding[i], max(1, left * loads[i] // whole), spare)
            holding[i] = holding[i] + addition
            spare = spare - addition
    return np.array([bound] + holding)


def uneven_parts(key, amount, total, bound, lean):
    if amount == 2:
        one = jax.random.randint(key, (), max(1, total - bound), min(bound, total - 1) + 1)
        return jnp.stack([one, total - one])
    sizes = jnp.asarray(length_profile(amount, total, bound, lean), jnp.int32)
    twos = (amount - 1) // 2
    giver, taker = sizes[1:1 + 2 * twos:2], sizes[2:2 + 2 * twos:2]
    slack = jnp.minimum(giver - 1, bound - taker)
    passed = jax.random.randint(jax.random.fold_in(key, 1), (twos,), 0, 1 << 20) % (slack + 1)
    sizes = sizes.at[1:1 + 2 * twos:2].set(giver - passed).at[2:2 + 2 * twos:2].set(taker + passed)
    return sizes[jax.random.permutation(jax.random.fold_in(key, 2), amount)]


def assign_block(rng, own, number, rows, number_of, top, most, lean):
    sequence = jax.random.permutation(rng, number_of)
    heavy_load, usual = portions_of(number_of, rows * top, most, lean, True), portions_of(number_of, rows * top, most, lean, False)
    places = jnp.arange(number_of)

    def named(sizes, offset_by):
        used = int((sizes > 0).sum())
        fixed = max(1, used // 4)
        passed = fixed + (places - fixed + offset_by * (used - fixed)) % max(1, number_of - fixed)
        return jnp.zeros((number_of,), jnp.int32).at[sequence[jnp.where(places < fixed, places, passed)]].set(jnp.asarray(sizes, jnp.int32))

    sizes = jnp.where(number % 4 == 0, named(heavy_load, number // 4), named(usual, number - number // 4 - 1))
    mixed = jax.random.permutation(jax.random.fold_in(own, 3), number_of)
    giver, sink = mixed[0:number_of // 2 * 2:2], mixed[1:number_of // 2 * 2:2]
    slack = jnp.minimum(sizes[giver] - 1, most - sizes[sink]) // 2
    slack = jnp.where((giver == sequence[0]) | (sink == sequence[0]) | (sizes[sink] == 0), 0, jnp.maximum(slack, 0))
    passed = jax.random.randint(jax.random.fold_in(own, 4), (number_of // 2,), 0, 1 << 20) % (slack + 1)
    sizes = sizes.at[giver].add(-passed).at[sink].add(passed)
    members = jnp.searchsorted(jnp.cumsum(sizes), jnp.arange(rows * top), side="right").astype(jnp.int32)
    listing = members.reshape(top, rows).T
    listing = listing[jax.random.permutation(jax.random.fold_in(own, 1), rows)]
    offset_by = jax.random.randint(jax.random.fold_in(own, 2), (rows, 1), 0, top)
    return jnp.take_along_axis(listing, (jnp.arange(top)[None, :] + offset_by) % top, axis=1)


def portions_of(count, total, reach, slope, full):
    loads = [(1 << 20) // math.isqrt(rank ** slope) + 1 for rank in range(1, count + 1)]
    largest = reach if full else min(reach, max(-(-total // count), total * loads[0] // sum(loads)))
    least = 1 if total - largest >= count - 1 else 0
    given, spare = [largest] + [least] * (count - 1), total - largest - least * (count - 1)
    while spare > 0:
        candidates = [i for i in range(1, count) if given[i] < largest] or [i for i in range(1, count) if given[i] < reach]
        mass, remaining = sum([loads[i] for i in candidates]), spare
        for i in candidates:
            more = min(reach - given[i], max(1, remaining * loads[i] // mass), spare)
            given[i] = given[i] + more
            spare = spare - more
    return np.array(given)


def gaussian(own_key, extent, deviation, most, cuts=(), held_as=jnp.bfloat16):
    level = steps_of(own_key, extent, cuts, -0.22, 0.18) if cuts else 1.0
    array = jax.random.normal(own_key, extent, jnp.float32) * deviation * level
    return jnp.minimum(jnp.maximum(array, -most), most).astype(held_as)


def setup_inputs(seed: int = 0) -> dict:
    arg_keys = jax.random.split(jax.random.key(seed), 18)
    queries = draw_queries(jax.random.fold_in(arg_keys[17], 71), 0)
    keys = draw_keys(jax.random.fold_in(arg_keys[17], 71), 0)
    values = gaussian(arg_keys[2], (KV_HEADS * HD, SEQUENCE_TOKENS), 1.0, 4.5, ((0, 2), (1, 64)))
    gate_cache = draw_gate_cache(jax.random.fold_in(arg_keys[17], 71), 0)
    documents = jnp.searchsorted(jnp.cumsum(uneven_parts(arg_keys[4], DOCS, SEQUENCE_TOKENS, DOC_MOST, 0)), jnp.arange(SEQUENCE_TOKENS), side="right").astype(jnp.int32)
    residual = gaussian(arg_keys[5], (SEQUENCE_TOKENS, D), 0.5, 3.0, ((0, 128),))
    out_weight = gaussian(arg_keys[6], (HEADS * HD, D), (4.0 / (HEADS * HD) ** 0.5), 2.0)
    mix_gain = jnp.clip(1.0 + 0.18 * jax.random.normal(arg_keys[7], (D,), jnp.float32), 0.099609375, 1.8984375).astype(jnp.bfloat16)
    routes_keys = jax.random.split(jax.random.fold_in(arg_keys[8], 1), SEQUENCE_TOKENS // ROWS)
    routes_turns = jax.random.permutation(jax.random.fold_in(arg_keys[8], 3), SEQUENCE_TOKENS // ROWS)
    routes = jax.vmap(lambda own, number: assign_block(jax.random.fold_in(arg_keys[8], 2), own, number, ROWS, EXPERTS, TOPK, CAP, 1))(routes_keys, routes_turns).reshape((SEQUENCE_TOKENS, TOPK))
    route_weight = jnp.clip(jnp.exp(math.log(1.0) - 1.3862944 * jax.random.uniform(arg_keys[9], (SEQUENCE_TOKENS, TOPK), jnp.float32) ** steps_of(arg_keys[9], (SEQUENCE_TOKENS, TOPK), ((0, 128),), -0.2, 0.2)), 0.25, 1.0)
    expert_gate = gaussian(arg_keys[10], (EXPERTS, D, EFF), D ** -0.5, 0.125, ((0, 128),))
    expert_up = gaussian(arg_keys[11], (EXPERTS, D, EFF), D ** -0.5, 0.125, ((0, 128),))
    expert_down = gaussian(arg_keys[12], (EXPERTS, EFF, D), EFF ** -0.5, 0.25, ((0, 128),))
    shared_gate = gaussian(arg_keys[13], (D, SFF), D ** -0.5, 0.125)
    shared_up = gaussian(arg_keys[14], (D, SFF), D ** -0.5, 0.125)
    shared_down = gaussian(arg_keys[15], (SFF, D), SFF ** -0.5, 0.25)
    ffn_gain = jnp.clip(1.0 + 0.18 * jax.random.normal(arg_keys[16], (D,), jnp.float32), 0.099609375, 1.8984375).astype(jnp.bfloat16)
    return dict(queries=queries, keys=keys, values=values, gate_cache=gate_cache, documents=documents, residual=residual, out_weight=out_weight, mix_gain=mix_gain, routes=routes, route_weight=route_weight, expert_gate=expert_gate, expert_up=expert_up, expert_down=expert_down, shared_gate=shared_gate, shared_up=shared_up, shared_down=shared_down, ffn_gain=ffn_gain)


residual_scale = 2.0 ** 0.25
norm_epsilon = 1e-05

def normalize(summed, gain_vector):
    row_mean = lax.optimization_barrier(jnp.mean(summed, axis=-1, keepdims=True))
    centred = summed - row_mean
    spread = lax.optimization_barrier(jnp.mean(centred * centred, axis=-1, keepdims=True))
    return (centred * lax.rsqrt(spread + norm_epsilon) * gain_vector.astype(jnp.float32)).astype(jnp.bfloat16)

def attend(queries, keys, values, gate_cache, documents):
    group_size = HEADS // KV_HEADS
    query_full = queries.astype(jnp.float32).reshape(SEQUENCE_TOKENS, KV_HEADS, group_size, HD)
    key_full = keys.astype(jnp.float32).reshape(KV_HEADS, HD, SEQUENCE_TOKENS)
    value_full = values.astype(jnp.float32).reshape(KV_HEADS, HD, SEQUENCE_TOKENS)
    cache = gate_cache.reshape(KV_HEADS, group_size, SEQUENCE_TOKENS)
    key_pos = jnp.arange(SEQUENCE_TOKENS, dtype=jnp.int32)
    score_scale = HD ** (-0.5)

    def block(block_index):
        first_row = (block_index * TOK_DEV).astype(jnp.int32)
        query_block = lax.dynamic_slice_in_dim(query_full, first_row, TOK_DEV, 0)
        query_cum = lax.dynamic_slice_in_dim(cache, first_row, TOK_DEV, 2)
        query_docs = lax.dynamic_slice_in_dim(documents, first_row, TOK_DEV, 0)
        scores = jnp.einsum('qagd,adk->qagk', query_block, key_full) * score_scale
        scores = scores + jnp.transpose(query_cum, (2, 0, 1))[..., None] - cache[None]
        query_pos = first_row + jnp.arange(TOK_DEV, dtype=jnp.int32)
        allowed = (key_pos[None, :] <= query_pos[:, None]) & (documents[None, :] == query_docs[:, None])
        allowed = allowed[:, None, None, :]
        highest = lax.optimization_barrier(jnp.max(jnp.where(allowed, scores, -jnp.inf), axis=-1, keepdims=True))
        weights = jnp.where(allowed, jnp.exp(scores - highest), 0.0)
        totals = lax.optimization_barrier(jnp.sum(weights, axis=-1))
        rounded = lax.optimization_barrier(weights.astype(jnp.bfloat16)).astype(jnp.float32)
        summed = jnp.einsum('qagk,adk->qagd', rounded, value_full)
        return (summed / totals[..., None]).astype(jnp.bfloat16).reshape(TOK_DEV, HEADS * HD)
    return lax.map(block, jnp.arange(SEQUENCE_TOKENS // TOK_DEV, dtype=jnp.int32)).reshape(SEQUENCE_TOKENS, HEADS * HD)

def experts_apply(settled, routes, route_weight, expert_gate, expert_up, expert_down):
    blocks = SEQUENCE_TOKENS // ROWS
    per_block = routes.reshape(blocks, ROWS * TOPK)
    matches = (per_block[:, :, None] == jnp.arange(EXPERTS, dtype=jnp.int32)[None, None, :]).astype(jnp.int32)
    ranks = lax.optimization_barrier(jnp.sum(jnp.cumsum(matches, axis=1) * matches, axis=2)) - 1
    block_ids = jnp.arange(blocks, dtype=jnp.int32)[:, None]
    slots = (per_block * blocks + block_ids) * CAP + ranks
    owners = block_ids * ROWS + jnp.arange(ROWS * TOPK, dtype=jnp.int32)[None, :] // TOPK
    table = jnp.zeros((EXPERTS * blocks * CAP,), jnp.int32).at[slots.reshape(-1)].set(owners.reshape(-1))
    table = table.reshape(EXPERTS, blocks * CAP)

    def one_expert(expert_index):
        taken = jnp.take(settled, table[expert_index], axis=0)
        gate_part = jnp.dot(taken, expert_gate[expert_index], preferred_element_type=jnp.float32)
        up_part = jnp.dot(taken, expert_up[expert_index], preferred_element_type=jnp.float32)
        hidden = (jax.nn.silu(gate_part) * up_part).astype(jnp.bfloat16)
        return jnp.dot(hidden, expert_down[expert_index], preferred_element_type=jnp.float32).astype(jnp.bfloat16)
    produced = lax.map(one_expert, jnp.arange(EXPERTS, dtype=jnp.int32)).reshape(EXPERTS * blocks * CAP, D)
    token_slots = slots.reshape(SEQUENCE_TOKENS, TOPK)
    routed = jnp.zeros((SEQUENCE_TOKENS, D), jnp.float32)
    for choice_index in range(TOPK):
        picked = jnp.take(produced, token_slots[:, choice_index], axis=0).astype(jnp.float32)
        routed = routed + picked * route_weight[:, choice_index][:, None]
    return routed

def reference(queries, keys, values, gate_cache, documents, residual, out_weight, mix_gain, routes, route_weight, expert_gate, expert_up, expert_down, shared_gate, shared_up, shared_down, ffn_gain):
    attended = attend(queries, keys, values, gate_cache, documents)
    mixed = jnp.dot(attended, out_weight, preferred_element_type=jnp.float32).astype(jnp.bfloat16)
    mixed = lax.optimization_barrier(mixed).astype(jnp.float32)
    settled = normalize(residual_scale * residual.astype(jnp.float32) + mixed, mix_gain)
    routed = experts_apply(settled, routes, route_weight, expert_gate, expert_up, expert_down)
    shared_gate_part = jnp.dot(settled, shared_gate, preferred_element_type=jnp.float32)
    shared_up_part = jnp.dot(settled, shared_up, preferred_element_type=jnp.float32)
    shared_hidden = (jax.nn.silu(shared_gate_part) * shared_up_part).astype(jnp.bfloat16)
    shared = jnp.dot(shared_hidden, shared_down, preferred_element_type=jnp.float32)
    return normalize(residual_scale * settled.astype(jnp.float32) + routed + shared, ffn_gain)
```

```python
import functools
import math

import jax
import jax.numpy as jnp
from jax import lax
from jax.experimental import pallas as pl
from jax.experimental.pallas import tpu as pltpu
from jax.sharding import Mesh, PartitionSpec as P

HD = 128
DOCS = 3
BIG = 2.0**100
residual_scale = 2.0**0.25
norm_epsilon = 1e-05
lowest = -1e30
tiny = 1e-30
root = math.sqrt(HD)
to_log2 = math.log2(math.e) / root


SP = ("z", "y", "x")
ALL = ("z", "y", "x", "tp")
VMEM = pl.BlockSpec(memory_space=pltpu.VMEM)
SMEM = pl.BlockSpec(memory_space=pltpu.SMEM)


def params(mib):
    return pltpu.CompilerParams(vmem_limit_bytes=mib << 20)


def three_pieces(v, cut):
    first = cut(v)
    second = cut(v - first)
    return first, second, cut(v - first - second)


def list_kernel(side, q0, q1, q2, q3, k0, k1, k2, k3, v0, v1, v2, v3, kact, vact, count):
    z, y, ks, vs = side[0], side[1], (k0, k1, k2, k3), (v0, v1, v2, v3)
    row = lax.broadcasted_iota(jnp.int32, (8, 512), 0)
    lane = lax.broadcasted_iota(jnp.int32, (8, 512), 1)
    pick = jnp.where((row == 6) & (lane == 256), 1.0, 0.0) + jnp.where(
        (row == 7) & (lane == 0), 2.0, 0.0
    )
    first = None
    for q in (q0, q1, q2, q3):
        doc = 3.0 - jnp.sum(q[256:264, :].astype(jnp.float32) * pick)
        first = doc if first is None else jnp.minimum(first, doc)
    row = lax.broadcasted_iota(jnp.int32, (16, 128), 0)
    lane = lax.broadcasted_iota(jnp.int32, (16, 128), 1)
    last_pick = jnp.where(lane == 127, jnp.where(row == 13, 1.0, jnp.where(row == 14, 2.0, 0.0)), 0.0)
    ones = jnp.where(lax.broadcasted_iota(jnp.int32, (112, 256), 0) < 2, 1.0, 0.0).astype(jnp.bfloat16)

    def put(slot, dz, dy):
        kact[slot, 0:144, :] = ks[dy][dz]
        kact[slot, 144:256, :] = ones
        vact[slot] = vs[dz][dy].T

    put(0, 0, 0)
    n = jnp.int32(1)
    for dz in range(4):
        for dy in range(4):
            if dz == 0 and dy == 0:
                continue
            last = 3.0 - jnp.sum(ks[dy][dz, 128:144, 128:256].astype(jnp.float32) * last_pick)
            other_y = lax.rem(y + dy, 4)
            before = (z >= dz) if dz else (other_y < y)
            needed = before & (last >= first)
            pl.when(needed)(functools.partial(put, n, dz, dy))
            n = n + needed.astype(jnp.int32)
    count[0] = n


def listed(side, qs, ks, vs):
    return pl.pallas_call(
        list_kernel,
        out_shape=(
            jax.ShapeDtypeStruct((16, 256, 256), jnp.bfloat16),
            jax.ShapeDtypeStruct((16, 256, 128), jnp.bfloat16),
            jax.ShapeDtypeStruct((1,), jnp.int32),
        ),
        in_specs=[SMEM] + [VMEM] * 12,
        out_specs=(VMEM, VMEM, SMEM),
        compiler_params=params(12),
        name="list_blocks",
    )(side, *qs, *ks, *vs)


def attend_kernel(own, side, count, q, w, kact, vact, same, other, qx, top, total, acc):
    x, tp, x_query = side[2], side[3], side[4]
    e = q[256:264, :].astype(jnp.float32)
    wide = jnp.concatenate(
        [e[:, 0:256], e[:, 256:512], jnp.zeros((112, 256), jnp.float32)], axis=0
    )
    columns = wide.T.astype(jnp.bfloat16)
    for h in range(4):
        qx[h, :, 0:128] = q[0:256, h * 128 : (h + 1) * 128]
        qx[h, :, 128:256] = jnp.dot(
            columns, w[h], preferred_element_type=jnp.float32
        ).astype(jnp.bfloat16)
    top[...] = jnp.full(top.shape, lowest, jnp.float32)
    total[...] = jnp.zeros(total.shape, jnp.float32)
    acc[...] = jnp.zeros(acc.shape, jnp.float32)

    def block(slot, diagonal):
        for h in range(4):
            s = jnp.dot(qx[h], kact[slot], preferred_element_type=jnp.float32)
            if diagonal:
                s = jnp.where(
                    lax.broadcasted_iota(jnp.int32, s.shape, 1)
                    <= lax.broadcasted_iota(jnp.int32, s.shape, 0),
                    s,
                    -BIG,
                )
            old = top[h]
            new = jnp.maximum(old, jnp.max(s, axis=1, keepdims=True) * to_log2)
            p = jnp.exp2(s * to_log2 - jnp.concatenate([new, new], axis=1))
            fade = jnp.exp2(old - new)
            top[h] = new
            total[h] = total[h] * fade + (p[:, 0:128] + p[:, 128:256])
            acc[h] = acc[h] * fade + jnp.dot(
                p.astype(jnp.bfloat16), vact[slot], preferred_element_type=jnp.float32
            )

    if own:
        block(0, True)
        start = jnp.int32(1)
    else:
        start = jnp.where(x_query > x, 0, 1).astype(jnp.int32)
    lax.fori_loop(start, count[0], lambda i, c: (block(i, False), c)[1], 0)

    row = lax.broadcasted_iota(jnp.int32, (8, 128), 0)
    cut = lambda v: v.astype(jnp.bfloat16).astype(jnp.float32)
    for ref, half in ((same, tp), (other, 1 - tp)):
        at = pl.multiple_of(half * 128, 128)
        for h in range(4):
            full = jnp.maximum(jnp.sum(total[h, pl.ds(at, 128), :], axis=1, keepdims=True), tiny)
            ref[0:128, h * 128 : (h + 1) * 128] = (acc[h, pl.ds(at, 128), :] / full).astype(
                jnp.bfloat16
            )
            level = (top[h, pl.ds(at, 128), :] + jnp.log2(full)).T[0:1, :]
            a, b, c = three_pieces(level, cut)
            ref[128:136, h * 128 : (h + 1) * 128] = jnp.where(
                row == 0, a, jnp.where(row == 1, b, jnp.where(row == 2, c, 0.0))
            ).astype(jnp.bfloat16)


def attended_part(own, side, count, q, w, kact, vact):
    shape = jax.ShapeDtypeStruct((136, 512), jnp.bfloat16)
    return pl.pallas_call(
        functools.partial(attend_kernel, own),
        out_shape=(shape, shape),
        in_specs=[SMEM, SMEM] + [VMEM] * 4,
        out_specs=(VMEM, VMEM),
        scratch_shapes=[
            pltpu.VMEM((4, 256, 256), jnp.bfloat16),
            pltpu.VMEM((4, 256, 128), jnp.float32),
            pltpu.VMEM((4, 256, 128), jnp.float32),
            pltpu.VMEM((4, 256, 128), jnp.float32),
        ],
        compiler_params=params(16),
        name="attend_own" if own else "attend",
    )(side, count, q, w, kact, vact)


def normalized(summed, gain):
    mean = jnp.mean(summed, axis=-1, keepdims=True)
    centred = summed - mean
    spread = jnp.mean(centred * centred, axis=-1, keepdims=True)
    return centred * lax.rsqrt(spread + norm_epsilon) * gain.astype(jnp.float32)


def mix_kernel(side, *refs):
    parts, (residual, out_weight, gain, placing, settled_out, sent) = refs[:8], refs[8:]
    tp = side[3]
    mixed = None
    for group, half in ((parts[0:4], tp), (parts[4:8], 1 - tp)):
        rows = []
        for r in group:
            stat = r[128:136, :].astype(jnp.float32)
            rows.append(stat[0:1] + stat[1:2] + stat[2:3])
        level = jnp.concatenate(rows + [rows[0]] * 4, axis=0)
        high = jnp.max(level, axis=0, keepdims=True)
        share = jnp.exp2(level - high)
        share = share / jnp.sum(share[0:4], axis=0, keepdims=True)
        heads = []
        for h in range(4):
            at = slice(h * 128, (h + 1) * 128)
            by_token = share[:, at].T
            heads.append(
                sum(
                    r[0:128, at].astype(jnp.float32) * by_token[:, i : i + 1]
                    for i, r in enumerate(group)
                ).astype(jnp.bfloat16)
            )
        part = jnp.dot(
            jnp.concatenate(heads, axis=1),
            out_weight[pl.ds(pl.multiple_of(half * 512, 512), 512), :],
            preferred_element_type=jnp.float32,
        )
        mixed = part if mixed is None else mixed + part
    mixed = mixed.astype(jnp.bfloat16).astype(jnp.float32)
    settled = normalized(
        residual_scale * residual[...].astype(jnp.float32) + mixed, gain[...]
    ).astype(jnp.bfloat16)
    settled_out[...] = settled
    for i in range(4):
        at = slice(i * 256, (i + 1) * 256)
        sent[at, :] = jnp.dot(
            placing[at, :], settled, preferred_element_type=jnp.float32
        ).astype(jnp.bfloat16)


def mix(side, parts, residual, out_weight, gain, placing):
    return pl.pallas_call(
        mix_kernel,
        out_shape=(
            jax.ShapeDtypeStruct((128, 2048), jnp.bfloat16),
            jax.ShapeDtypeStruct((1024, 2048), jnp.bfloat16),
        ),
        in_specs=[SMEM] + [VMEM] * 12,
        out_specs=(VMEM, VMEM),
        compiler_params=params(24),
        name="mix",
    )(side, *parts, residual, out_weight, gain, placing)


def swish(v):
    return v / (1.0 + jnp.exp(-v))


def expert_kernel(rows, gate, up, down, out):
    x = rows[...]
    g = jnp.dot(x, gate[...], preferred_element_type=jnp.float32)
    u = jnp.dot(x, up[...], preferred_element_type=jnp.float32)
    hidden = (swish(g) * u).astype(jnp.bfloat16)
    out[...] = jnp.dot(hidden, down[...], preferred_element_type=jnp.float32).astype(out.dtype)


def feed_forward(rows, gate, up, down, step, dtype, name):
    n, d = rows.shape
    return pl.pallas_call(
        expert_kernel,
        grid=(n // step,),
        out_shape=jax.ShapeDtypeStruct((n, d), dtype),
        in_specs=[
            pl.BlockSpec((step, d), lambda i: (i, 0)),
            pl.BlockSpec(gate.shape, lambda i: (0, 0)),
            pl.BlockSpec(up.shape, lambda i: (0, 0)),
            pl.BlockSpec(down.shape, lambda i: (0, 0)),
        ],
        out_specs=pl.BlockSpec((step, d), lambda i: (i, 0)),
        compiler_params=params(32),
        name=name,
    )(rows, gate, up, down)


def final_kernel(returned, high, low, settled, shared, gain, out):
    routed = jnp.dot(high[...], returned[...], preferred_element_type=jnp.float32)
    routed = routed + jnp.dot(low[...], returned[...], preferred_element_type=jnp.float32)
    summed = residual_scale * settled[...].astype(jnp.float32) + routed + shared[...]
    out[...] = normalized(summed, gain[...]).astype(jnp.bfloat16)


def finish(returned, high, low, settled, shared, gain):
    return pl.pallas_call(
        final_kernel,
        out_shape=jax.ShapeDtypeStruct((128, 2048), jnp.bfloat16),
        in_specs=[VMEM] * 6,
        out_specs=VMEM,
        compiler_params=params(24),
        name="finish",
    )(returned, high, low, settled, shared, gain)


def from_next(array, axis, step):
    return lax.ppermute(array, axis, [((i + step) % 4, i) for i in range(4)])


def from_before(array, axis, step):
    return lax.ppermute(array, axis, [(i - step, i) for i in range(step, 4)])


def widening():
    order = [2 * i for i in range(8)] + [2 * i + 1 for i in range(8)]
    rows = []
    for h in range(4):
        table = [[0.0] * 128 for _ in range(16)]
        for p in range(3):
            table[p * 4 + h][15 + p] = 1.0
            table[15][p * 4 + h] = -1.0
        for d in range(DOCS):
            table[15][12 + d] = -BIG
            table[12 + d][12 + d] = BIG
        rows.append([table[r] for r in order] + [[0.0] * 128 for _ in range(112)])
    return jnp.array(rows, jnp.bfloat16)


def local(
    queries,
    keys,
    values,
    gate_cache,
    documents,
    residual,
    out_weight,
    mix_gain,
    routes,
    route_weight,
    expert_gate,
    expert_up,
    expert_down,
    shared_gate,
    shared_up,
    shared_down,
    ffn_gain,
):
    z, y, x, tp = (lax.axis_index(a) for a in ALL)
    cut = lambda v: lax.reduce_precision(v, 8, 7)
    pieces = three_pieces(gate_cache * root, cut)
    elsewhere = documents[None, :] != jnp.arange(DOCS, dtype=jnp.int32)[:, None]
    extra = jnp.concatenate(
        [*pieces, elsewhere.astype(jnp.float32), jnp.ones((1, 256), jnp.float32)], axis=0
    ).astype(jnp.bfloat16)

    key_rows = jnp.concatenate([keys, extra], axis=0)
    query_rows = jnp.concatenate([queries, extra.reshape(8, 512)], axis=0)
    key_line = jnp.stack([key_rows] + [from_before(key_rows, "z", s) for s in (1, 2, 3)])
    value_line = jnp.stack([values] + [from_next(values, "y", s) for s in (1, 2, 3)])
    group = [query_rows] + [from_next(query_rows, "x", s) for s in (1, 2, 3)]
    key_parts = [key_line] + [from_next(key_line, "y", s) for s in (1, 2, 3)]
    value_parts = [value_line] + [from_before(value_line, "z", s) for s in (1, 2, 3)]

    side = lambda j: jnp.stack([z, y, x, tp, lax.rem(x + j, 4)]).astype(jnp.int32)
    kact, vact, count = listed(side(0), group, key_parts, value_parts)
    w = widening()
    same, other = [None] * 4, [None] * 4
    for j in (2, 1, 3, 0):
        mine, partner = attended_part(j == 0, side(j), count, group[j], w, kact, vact)
        to_same = [((a * 2 + t), ((a + j) % 4) * 2 + t) for a in range(4) for t in range(2)]
        to_other = [((a * 2 + t), ((a + j) % 4) * 2 + 1 - t) for a in range(4) for t in range(2)]
        same[j] = mine if j == 0 else lax.ppermute(mine, ("x", "tp"), to_same)
        other[j] = lax.ppermute(partner, ("x", "tp"), to_other)

    tokens, top_count = routes.shape
    width = residual.shape[1]
    experts = lax.axis_size(ALL)
    capacity = tokens * 2 * top_count // experts
    slot_total = experts * capacity
    chosen = routes.reshape(-1)
    pairs = chosen.shape[0]
    matches = (chosen[:, None] == jnp.arange(experts, dtype=jnp.int32)[None, :]).astype(jnp.bfloat16)
    earlier = (jnp.arange(pairs)[None, :] < jnp.arange(pairs)[:, None]).astype(jnp.bfloat16)
    before = jnp.dot(earlier, matches, preferred_element_type=jnp.float32)
    ranks = jnp.sum(before * matches.astype(jnp.float32), axis=1).astype(jnp.int32)
    slots = (chosen * capacity + ranks).reshape(tokens, top_count)
    every = jnp.arange(slot_total, dtype=jnp.int32)
    placing = sum(
        (slots[:, k][None, :] == every[:, None]).astype(jnp.float32) for k in range(top_count)
    ).astype(jnp.bfloat16)
    picking = sum(
        jnp.where(slots[:, k : k + 1] == every[None, :], route_weight[:, k : k + 1], 0.0)
        for k in range(top_count)
    )
    high = cut(picking)
    low = (picking - high).astype(jnp.bfloat16)
    high = high.astype(jnp.bfloat16)

    settled, sent = mix(
        side(0), [*same, *other], residual, out_weight, mix_gain.reshape(1, width), placing
    )
    arrived = lax.all_to_all(
        sent.reshape(experts, capacity, width), ALL, split_axis=0, concat_axis=0, tiled=True
    )
    shared = feed_forward(
        settled, shared_gate, shared_up, shared_down, 128, jnp.float32, "shared"
    )
    finished = feed_forward(
        arrived.reshape(slot_total, width),
        expert_gate[0],
        expert_up[0],
        expert_down[0],
        256,
        jnp.bfloat16,
        "experts",
    )
    returned = lax.all_to_all(
        finished.reshape(experts, capacity, width), ALL, split_axis=0, concat_axis=0, tiled=True
    )
    return finish(
        returned.reshape(slot_total, width), high, low, settled, shared, ffn_gain.reshape(1, width)
    )


def solution(mesh):
    grid = Mesh(mesh.devices.reshape(4, 4, 4, 2), ALL)
    placed = (
        P(SP, "tp"),
        P("tp", SP),
        P("tp", SP),
        P("tp", SP),
        P(SP),
        P(ALL, None),
        P(),
        P(),
        P(ALL, None),
        P(ALL, None),
        P(ALL, None, None),
        P(ALL, None, None),
        P(ALL, None, None),
        P(),
        P(),
        P(),
        P(),
    )
    return jax.shard_map(
        local, mesh=grid, in_specs=placed, out_specs=P(ALL, None), check_vma=False
    )
```

```python
import functools
import math

import jax
import jax.numpy as jnp
from jax import lax
from jax.experimental import pallas as pl
from jax.experimental.pallas import tpu as pltpu
from jax.sharding import Mesh, PartitionSpec as P

HD = 128
DOCS = 3
BIG = 2.0**100
residual_scale = 2.0**0.25
norm_epsilon = 1e-05
lowest = -1e30
tiny = 1e-30
root = math.sqrt(HD)
to_log2 = math.log2(math.e) / root


SP = ("z", "y", "x")
ALL = ("z", "y", "x", "tp")
VMEM = pl.BlockSpec(memory_space=pltpu.VMEM)
SMEM = pl.BlockSpec(memory_space=pltpu.SMEM)


def params(mib):
    return pltpu.CompilerParams(vmem_limit_bytes=mib << 20)


def three_pieces(v, cut):
    first = cut(v)
    second = cut(v - first)
    return first, second, cut(v - first - second)


def list_kernel(side, q0, q1, q2, q3, k0, k1, k2, k3, v0, v1, v2, v3, kact, vact, count):
    z, y, ks, vs = side[0], side[1], (k0, k1, k2, k3), (v0, v1, v2, v3)
    row = lax.broadcasted_iota(jnp.int32, (8, 512), 0)
    lane = lax.broadcasted_iota(jnp.int32, (8, 512), 1)
    pick = jnp.where((row == 6) & (lane == 256), 1.0, 0.0) + jnp.where(
        (row == 7) & (lane == 0), 2.0, 0.0
    )
    firsts = [3.0 - jnp.sum(q[256:264, :].astype(jnp.float32) * pick) for q in (q0, q1, q2, q3)]
    row = lax.broadcasted_iota(jnp.int32, (16, 128), 0)
    lane = lax.broadcasted_iota(jnp.int32, (16, 128), 1)
    last_pick = jnp.where(lane == 127, jnp.where(row == 13, 1.0, jnp.where(row == 14, 2.0, 0.0)), 0.0)
    others = [(dz, dy) for dz in range(4) for dy in range(4) if dz or dy]
    lasts = [
        3.0 - jnp.sum(ks[dy][dz, 128:144, 128:256].astype(jnp.float32) * last_pick)
        for dz, dy in others
    ]
    first = jnp.minimum(jnp.minimum(firsts[0], firsts[1]), jnp.minimum(firsts[2], firsts[3]))
    row = lax.broadcasted_iota(jnp.int32, (112, 256), 0)
    ones = jnp.where(row < 2, 1.0, 0.0).astype(jnp.bfloat16)

    def put(slot, dz, dy):
        kact[slot, 0:144, :] = ks[dy][dz]
        kact[slot, 144:256, :] = ones
        vact[slot] = vs[dz][dy].T

    put(0, 0, 0)
    n = jnp.int32(1)
    for (dz, dy), last in zip(others, lasts):
        before = (z >= dz) if dz else (lax.rem(y + dy, 4) < y)
        needed = before & (last >= first)
        pl.when(needed)(functools.partial(put, n, dz, dy))
        n = n + needed.astype(jnp.int32)
    row = lax.broadcasted_iota(jnp.int32, (256, 256), 0)
    kact[n] = jnp.where((row >= 140) & (row < 143), 1.0, 0.0).astype(jnp.bfloat16)
    vact[n] = jnp.zeros((256, 128), jnp.bfloat16)
    count[0] = n


SLOTS = 12


def listed(side, qs, ks, vs):
    return pl.pallas_call(
        list_kernel,
        out_shape=(
            jax.ShapeDtypeStruct((SLOTS, 256, 256), jnp.bfloat16),
            jax.ShapeDtypeStruct((SLOTS, 256, 128), jnp.bfloat16),
            jax.ShapeDtypeStruct((1,), jnp.int32),
        ),
        in_specs=[SMEM] + [VMEM] * 12,
        out_specs=(VMEM, VMEM, SMEM),
        compiler_params=params(12),
        name="list_blocks",
    )(side, *qs, *ks, *vs)


def attend_kernel(steps, side, count, *refs):
    n = len(steps)
    qs, (w, kact, vact), outs = refs[:n], refs[n : n + 3], refs[n + 3 : 3 * n + 3]
    qx, top, total, acc, scores = refs[3 * n + 3 :]
    x, tp = side[2], side[3]
    for b, q in enumerate(qs):
        e = q[256:264, :].astype(jnp.float32)
        wide = jnp.concatenate(
            [e[:, 0:256], e[:, 256:512], jnp.zeros((112, 256), jnp.float32)], axis=0
        )
        columns = wide.T.astype(jnp.bfloat16)
        for h in range(4):
            at = slice((b * 4 + h) * 256, (b * 4 + h + 1) * 256)
            qx[at, 0:128] = q[0:256, h * 128 : (h + 1) * 128]
            qx[at, 128:256] = jnp.dot(columns, w[h], preferred_element_type=jnp.float32).astype(
                jnp.bfloat16
            )
    top[...] = jnp.full(top.shape, lowest, jnp.float32)
    total[...] = jnp.zeros(total.shape, jnp.float32)
    acc[...] = jnp.zeros(acc.shape, jnp.float32)

    def score(i, masked):
        for b, step in enumerate(steps):
            at = slice(b * 1024, (b + 1) * 1024)
            left = jnp.dot(qx[at, :], kact[2 * i], preferred_element_type=jnp.float32) * to_log2
            if masked:
                ahead = (lax.rem(x + step, 4) - x) * 256
                row = lax.broadcasted_iota(jnp.int32, left.shape, 0)
                column = lax.broadcasted_iota(jnp.int32, left.shape, 1)
                left = jnp.where(column <= lax.rem(row, 256) + ahead, left, -BIG)
            right = jnp.dot(qx[at, :], kact[2 * i + 1], preferred_element_type=jnp.float32) * to_log2
            scores[i, at, 0:256] = left
            scores[i, at, 256:512] = right
            high = jnp.maximum(left, right)
            top[at, :] = jnp.maximum(top[at, :], jnp.maximum(high[:, 0:128], high[:, 128:256]))

    def add(i):
        v = vact[pl.ds(2 * i, 2)].reshape(512, 128)
        for r in range(0, n * 1024, 256):
            at = slice(r, r + 256)
            high = top[at, :]
            p = [jnp.exp2(scores[i, at, c : c + 128] - high) for c in range(0, 512, 128)]
            total[at, :] += (p[0] + p[1]) + (p[2] + p[3])
            low = jnp.concatenate([part.astype(jnp.bfloat16) for part in p], axis=1)
            acc[at, :] += jnp.dot(low, v, preferred_element_type=jnp.float32)

    pairs = lax.div(count[0] + 1, 2)
    score(0, True)
    lax.fori_loop(1, pairs, lambda i, c: (score(i, False), c)[1], 0)
    top[...] = jnp.broadcast_to(jnp.max(top[...], axis=1, keepdims=True), top.shape)
    lax.fori_loop(0, pairs, lambda i, c: (add(i), c)[1], 0)

    row = lax.broadcasted_iota(jnp.int32, (8, 128), 0)
    cut = lambda v: v.astype(jnp.bfloat16).astype(jnp.float32)
    for b in range(n):
        for ref, half in ((outs[2 * b], tp), (outs[2 * b + 1], 1 - tp)):
            for h in range(4):
                at = pl.ds(pl.multiple_of(half * 128 + (b * 4 + h) * 256, 128), 128)
                full = jnp.maximum(jnp.sum(total[at, :], axis=1, keepdims=True), tiny)
                ref[0:128, h * 128 : (h + 1) * 128] = (acc[at, :] / full).astype(jnp.bfloat16)
                level = (top[at, :] + jnp.log2(full)).T[0:1, :]
                p0, p1, p2 = three_pieces(level, cut)
                ref[128:136, h * 128 : (h + 1) * 128] = jnp.where(
                    row == 0, p0, jnp.where(row == 1, p1, jnp.where(row == 2, p2, 0.0))
                ).astype(jnp.bfloat16)


def attended_parts(steps, side, count, qs, w, kact, vact):
    n = len(steps)
    shape = jax.ShapeDtypeStruct((136, 512), jnp.bfloat16)
    return pl.pallas_call(
        functools.partial(attend_kernel, steps),
        out_shape=(shape,) * (2 * n),
        in_specs=[SMEM, SMEM] + [VMEM] * (n + 3),
        out_specs=(VMEM,) * (2 * n),
        scratch_shapes=[
            pltpu.VMEM((n * 1024, 256), jnp.bfloat16),
            pltpu.VMEM((n * 1024, 128), jnp.float32),
            pltpu.VMEM((n * 1024, 128), jnp.float32),
            pltpu.VMEM((n * 1024, 128), jnp.float32),
            pltpu.VMEM((SLOTS // 2, n * 1024, 512), jnp.float32),
        ],
        compiler_params=params(8 + 16 * n),
        name="attend_" + "".join(map(str, steps)),
    )(side, count, *qs, w, kact, vact)


def normalized(summed, gain):
    mean = jnp.mean(summed, axis=-1, keepdims=True)
    centred = summed - mean
    spread = jnp.mean(centred * centred, axis=-1, keepdims=True)
    return centred * lax.rsqrt(spread + norm_epsilon) * gain.astype(jnp.float32)


def mix_kernel(side, *refs):
    parts, (residual, out_weight, gain, slots, settled_out, sent) = refs[:8], refs[8:]
    tp = side[3]
    mixed = None
    for group, half in ((parts[0:4], tp), (parts[4:8], 1 - tp)):
        rows = []
        for r in group:
            stat = r[128:136, :].astype(jnp.float32)
            rows.append(stat[0:1] + stat[1:2] + stat[2:3])
        level = jnp.concatenate(rows + [rows[0]] * 4, axis=0)
        high = jnp.max(level, axis=0, keepdims=True)
        share = jnp.exp2(level - high)
        share = share / jnp.sum(share[0:4], axis=0, keepdims=True)
        heads = []
        for h in range(4):
            at = slice(h * 128, (h + 1) * 128)
            by_token = share[:, at].T
            heads.append(
                sum(
                    r[0:128, at].astype(jnp.float32) * by_token[:, i : i + 1]
                    for i, r in enumerate(group)
                ).astype(jnp.bfloat16)
            )
        part = jnp.dot(
            jnp.concatenate(heads, axis=1),
            out_weight[pl.ds(pl.multiple_of(half * 512, 512), 512), :],
            preferred_element_type=jnp.float32,
        )
        mixed = part if mixed is None else mixed + part
    mixed = mixed.astype(jnp.bfloat16).astype(jnp.float32)
    settled = normalized(
        residual_scale * residual[...].astype(jnp.float32) + mixed, gain[...]
    ).astype(jnp.bfloat16)
    settled_out[...] = settled
    for at in range(0, 1024, 256):
        every = lax.broadcasted_iota(jnp.int32, (256, 128), 0) + at
        held = every == slots[0:1, :]
        for k in range(1, slots.shape[0]):
            held = held | (every == slots[k : k + 1, :])
        placing = jnp.where(held, 1.0, 0.0).astype(jnp.bfloat16)
        sent[at : at + 256, :] = jnp.dot(
            placing, settled, preferred_element_type=jnp.float32
        ).astype(jnp.bfloat16)


def mix(side, parts, residual, out_weight, gain, slots):
    return pl.pallas_call(
        mix_kernel,
        out_shape=(
            jax.ShapeDtypeStruct((128, 2048), jnp.bfloat16),
            jax.ShapeDtypeStruct((1024, 2048), jnp.bfloat16),
        ),
        in_specs=[SMEM] + [VMEM] * 12,
        out_specs=(VMEM, VMEM),
        compiler_params=params(24),
        name="mix",
    )(side, *parts, residual, out_weight, gain, slots)


def swish(v):
    return v / (1.0 + jnp.exp(-v))


def expert_kernel(rows, gate, up, down, out):
    x = rows[...]
    g = jnp.dot(x, gate[...], preferred_element_type=jnp.float32)
    u = jnp.dot(x, up[...], preferred_element_type=jnp.float32)
    hidden = (swish(g) * u).astype(jnp.bfloat16)
    out[...] = jnp.dot(hidden, down[...], preferred_element_type=jnp.float32).astype(out.dtype)


def feed_forward(rows, gate, up, down, step):
    n, d = rows.shape
    return pl.pallas_call(
        expert_kernel,
        grid=(n // step,),
        out_shape=jax.ShapeDtypeStruct((n, d), jnp.bfloat16),
        in_specs=[
            pl.BlockSpec((step, d), lambda i: (i, 0)),
            pl.BlockSpec(gate.shape, lambda i: (0, 0)),
            pl.BlockSpec(up.shape, lambda i: (0, 0)),
            pl.BlockSpec(down.shape, lambda i: (0, 0)),
        ],
        out_specs=pl.BlockSpec((step, d), lambda i: (i, 0)),
        compiler_params=params(32),
        name="experts",
    )(rows, gate, up, down)


def final_kernel(returned, slots, weights, settled, gate, up, down, gain, out):
    x = settled[...]
    g = jnp.dot(x, gate[...], preferred_element_type=jnp.float32)
    u = jnp.dot(x, up[...], preferred_element_type=jnp.float32)
    hidden = (swish(g) * u).astype(jnp.bfloat16)
    shared = jnp.dot(hidden, down[...], preferred_element_type=jnp.float32)
    every = lax.broadcasted_iota(jnp.int32, (128, 1024), 1)
    picking = jnp.zeros((128, 1024), jnp.float32)
    for k in range(slots.shape[1]):
        picking = jnp.where(every == slots[:, k : k + 1], weights[:, k : k + 1], picking)
    high = picking.astype(jnp.bfloat16)
    low = (picking - high.astype(jnp.float32)).astype(jnp.bfloat16)
    both = jnp.dot(
        jnp.concatenate([high, low], axis=0), returned[...], preferred_element_type=jnp.float32
    )
    routed = both[0:128] + both[128:256]
    summed = residual_scale * x.astype(jnp.float32) + routed + shared
    out[...] = normalized(summed, gain[...]).astype(jnp.bfloat16)


def finish(returned, slots, weights, settled, gate, up, down, gain):
    return pl.pallas_call(
        final_kernel,
        out_shape=jax.ShapeDtypeStruct((128, 2048), jnp.bfloat16),
        in_specs=[VMEM] * 8,
        out_specs=VMEM,
        compiler_params=params(24),
        name="finish",
    )(returned, slots, weights, settled, gate, up, down, gain)


def from_next(array, axis, step):
    return lax.ppermute(array, axis, [((i + step) % 4, i) for i in range(4)])


def from_before(array, axis, step):
    return lax.ppermute(array, axis, [(i - step, i) for i in range(step, 4)])


def widening():
    order = [2 * i for i in range(8)] + [2 * i + 1 for i in range(8)]
    rows = []
    for h in range(4):
        table = [[0.0] * 128 for _ in range(16)]
        for p in range(3):
            table[p * 4 + h][15 + p] = 1.0
            table[15][p * 4 + h] = -1.0
        for d in range(DOCS):
            table[15][12 + d] = -BIG
            table[12 + d][12 + d] = BIG
        rows.append([table[r] for r in order] + [[0.0] * 128 for _ in range(112)])
    return jnp.array(rows, jnp.bfloat16)


def local(
    queries,
    keys,
    values,
    gate_cache,
    documents,
    residual,
    out_weight,
    mix_gain,
    routes,
    route_weight,
    expert_gate,
    expert_up,
    expert_down,
    shared_gate,
    shared_up,
    shared_down,
    ffn_gain,
):
    z, y, x, tp = (lax.axis_index(a) for a in ALL)
    cut = lambda v: lax.reduce_precision(v, 8, 7)
    pieces = three_pieces(gate_cache * root, cut)
    elsewhere = documents[None, :] != jnp.arange(DOCS, dtype=jnp.int32)[:, None]
    extra = jnp.concatenate(
        [*pieces, elsewhere.astype(jnp.float32), jnp.ones((1, 256), jnp.float32)], axis=0
    ).astype(jnp.bfloat16)

    key_rows = jnp.concatenate([keys, extra], axis=0)
    query_rows = jnp.concatenate([queries, extra.reshape(8, 512)], axis=0)
    key_line = jnp.stack([key_rows] + [from_before(key_rows, "z", s) for s in (1, 2, 3)])
    value_line = jnp.stack([values] + [from_next(values, "y", s) for s in (1, 2, 3)])
    query_rows, key_line, value_line = lax.optimization_barrier(
        (query_rows, key_line, value_line)
    )
    key_parts = [key_line] + [from_next(key_line, "y", s) for s in (1, 2, 3)]
    value_parts = [value_line] + [from_before(value_line, "z", s) for s in (1, 2, 3)]
    group = [query_rows] + [from_next(query_rows, "x", s) for s in (1, 2, 3)]

    side = jnp.stack([z, y, x, tp]).astype(jnp.int32)
    kact, vact, count = listed(side, group, key_parts, value_parts)
    w = widening()
    same, other = [None] * 4, [None] * 4
    for steps in ((2, 1), (3, 0)):
        parts = attended_parts(steps, side, count, [group[j] for j in steps], w, kact, vact)
        for b, j in enumerate(steps):
            line = [(a, t) for a in range(4) for t in range(2)]
            to_same = [(a * 2 + t, ((a + j) % 4) * 2 + t) for a, t in line]
            to_other = [(a * 2 + t, ((a + j) % 4) * 2 + 1 - t) for a, t in line]
            mine, partner = parts[2 * b], parts[2 * b + 1]
            same[j] = mine if j == 0 else lax.ppermute(mine, ("x", "tp"), to_same)
            other[j] = lax.ppermute(partner, ("x", "tp"), to_other)

    tokens, top_count = routes.shape
    width = residual.shape[1]
    experts = lax.axis_size(ALL)
    capacity = tokens * 2 * top_count // experts
    slot_total = experts * capacity
    chosen = routes.reshape(-1)
    pairs = chosen.shape[0]
    matches = (chosen[:, None] == jnp.arange(experts, dtype=jnp.int32)[None, :]).astype(jnp.bfloat16)
    earlier = (jnp.arange(pairs)[None, :] < jnp.arange(pairs)[:, None]).astype(jnp.bfloat16)
    before = jnp.dot(earlier, matches, preferred_element_type=jnp.float32)
    ranks = jnp.sum(before * matches.astype(jnp.float32), axis=1).astype(jnp.int32)
    slots = (chosen * capacity + ranks).reshape(tokens, top_count)

    settled, sent = mix(
        side, [*same, *other], residual, out_weight, mix_gain.reshape(1, width), slots.T
    )
    arrived = lax.all_to_all(
        sent.reshape(experts, capacity, width), ALL, split_axis=0, concat_axis=0, tiled=True
    )
    finished = feed_forward(
        arrived.reshape(slot_total, width), expert_gate[0], expert_up[0], expert_down[0], 256
    )
    returned = lax.all_to_all(
        finished.reshape(experts, capacity, width), ALL, split_axis=0, concat_axis=0, tiled=True
    )
    return finish(
        returned.reshape(slot_total, width),
        slots,
        route_weight,
        settled,
        shared_gate,
        shared_up,
        shared_down,
        ffn_gain.reshape(1, width),
    )


def solution(mesh):
    grid = Mesh(mesh.devices.reshape(4, 4, 4, 2), ALL)
    placed = (
        P(SP, "tp"),
        P("tp", SP),
        P("tp", SP),
        P("tp", SP),
        P(SP),
        P(ALL, None),
        P(),
        P(),
        P(ALL, None),
        P(ALL, None),
        P(ALL, None, None),
        P(ALL, None, None),
        P(ALL, None, None),
        P(),
        P(),
        P(),
        P(),
    )
    return jax.shard_map(
        local, mesh=grid, in_specs=placed, out_specs=P(ALL, None), check_vma=False
    )
```
